32 devices in a mesh: sp: 8 (over z, x), tp: 4 (over y, core).
Axes of the slice: x: 2, y: 2, z: 4, core: 2. Of those that a mesh axis runs over, the one named last changes fastest.
Arguments:
- tokens: bfloat16 [3072, 2048], P('sp', 'tp'), may hold values from -6 to 6
- norm_gain: float32 [2048], replicated, may hold values from 0.1 to 1.9
- w_pool_in: bfloat16 [2048, 2048], P('sp', 'tp'), may hold values from -0.125 to 0.125
- w_lru_in: bfloat16 [2048, 2048], P('sp', 'tp'), may hold values from -0.125 to 0.125
- pool_mix: bfloat16 [4, 512, 512], P('tp'), may hold values from -0.25 to 0.25
- conv_taps: bfloat16 [4, 2048], P(None, 'tp'), may hold values from -3 to 3
- rec_gate: bfloat16 [2, 16, 128, 128], P(None, 'tp'), may hold values from -0.5 to 0.5
- in_gate: bfloat16 [2, 16, 128, 128], P(None, 'tp'), may hold values from -0.5 to 0.5
- decay_rate: float32 [2, 2048], P(None, 'tp'), may hold values from 0 to 1, as said below
- log_decay: float32 [2, 3072], P(None, 'sp'), may hold values from -2 to 0, as said below
- start_state: float32 [2, 2048], P(None, 'tp'), may hold values from -8 to 8
- w_out_pool: bfloat16 [2048, 2048], P('tp', 'sp'), may hold values from -0.09375 to 0.09375
- w_out_lru: bfloat16 [2048, 2048], P('tp', 'sp'), may hold values from -0.09375 to 0.09375
Outputs:
- mixed: bfloat16 [3072, 2048], P(('sp', 'tp'))
The draws below stay inside these ranges and needn't reach their ends.
Inputs may be any that keep to these rules, and one draw needn't show every extreme that they name: `decay_rate`: positive. `log_decay`: at most zero.
All inputs are finite; a program needn't handle non-finite values.
Results may differ from the reference program's by a relative error of at most 0.0068.
Values may be sent and summed in bfloat16 or wider, within the bound.
A program may use at most 64 MiB of HBM per device.

```python
import math
import jax
import jax.numpy as jnp
from jax import lax

D = 2048
D_POOL = 2048
POOL_GROUPS = 4
GROUP_W = 512
D_LRU = 2048
HEAD = 128
BLOCKS = 16
CONV = 4
GRID_W = 32
TOKENS = 3072
ROWS = 96


def draw_decay_rate(key, part):
    pick_key, slow_key, fast_key = jax.random.split(jax.random.fold_in(key, 11), 3)
    slow_rate = jnp.exp(jax.random.uniform(slow_key, (2, D_LRU), jnp.float32, math.log(0.02), math.log(0.1))) / TOKENS
    fast_rate = jnp.exp(jax.random.uniform(fast_key, (2, D_LRU), jnp.float32, math.log(1.0 / 400.0), math.log(1.0 / 120.0)))
    share = 0.5
    chosen = jax.random.uniform(pick_key, (2, D_LRU), jnp.float32) < share
    return jnp.where(chosen, fast_rate, slow_rate).astype(jnp.float32)


def draw_log_decay(key, part):
    rate_key, place_key, depth_key = jax.random.split(jax.random.fold_in(key, 23), 3)
    lower_rate = 0.2
    upper_rate = 0.8
    grid_rows = TOKENS // GRID_W
    row_rates = jnp.exp(jax.random.uniform(rate_key, (2, grid_rows), jnp.float32, math.log(lower_rate), math.log(upper_rate))) / TOKENS
    equilibrium_hidden = -jnp.repeat(row_rates, GRID_W, axis=1)
    element_slots = jax.random.randint(place_key, (2, 3), 0, TOKENS)
    layer_counts_drawn = jax.random.uniform(depth_key, (2, 3), jnp.float32, math.log(0.5), math.log(0.8))
    element_offsets = jnp.arange(TOKENS, dtype=jnp.int32)
    segment_extents = jnp.sum((element_offsets[None, None, :] == element_slots[:, :, None]).astype(jnp.float32) * layer_counts_drawn[:, :, None], axis=1)
    return (equilibrium_hidden + segment_extents).astype(jnp.float32)


def block_levels(stream_key, shape, pieces, least, top_value):
    gain, own = 1.0, jax.random.fold_in(stream_key, 6)
    for position, shards_of in pieces:
        draws = jnp.exp(jax.random.uniform(jax.random.fold_in(own, position), (shards_of,), jnp.float32, least / len(pieces), top_value / len(pieces)))
        gain = gain * jnp.repeat(draws, shape[position] // shards_of).reshape([-1 if axis == position else 1 for axis in range(len(shape))])
    return gain


def noise(own_key, shape, width, reach, pieces=(), kind=jnp.bfloat16):
    values = jax.random.normal(own_key, shape, jnp.float32) * width
    if len(pieces) > 0:
        values = block_levels(own_key, shape, pieces, -0.22, 0.18) * values
    return jnp.clip(values, min=-reach, max=reach).astype(kind)


def setup_inputs(seed: int = 0) -> dict:
    streams_of = jax.random.split(jax.random.key(seed), 14)
    tokens = noise(streams_of[0], (TOKENS, D), 1.0, 6.0, ((0, 8), (1, 4)))
    norm_gain = jnp.clip(1.0 + 0.18 * jax.random.normal(streams_of[1], (D,), jnp.float32), 0.1, 1.9)
    w_pool_in = noise(streams_of[2], (D, D_POOL), D ** -0.5, 0.125, ((0, 8), (1, 4)))
    w_lru_in = noise(streams_of[3], (D, D_LRU), D ** -0.5, 0.125, ((0, 8), (1, 4)))
    pool_mix = noise(streams_of[4], (POOL_GROUPS, GROUP_W, GROUP_W), GROUP_W ** -0.5, 0.25, ((0, 4),))
    conv_taps = noise(streams_of[5], (CONV, D_LRU), 0.5, 3.0, ((1, 4),))
    rec_gate = noise(streams_of[6], (2, BLOCKS, HEAD, HEAD), HEAD ** -0.5, 0.5, ((1, 4),))
    in_gate = noise(streams_of[7], (2, BLOCKS, HEAD, HEAD), HEAD ** -0.5, 0.5, ((1, 4),))
    decay_rate = draw_decay_rate(jax.random.fold_in(streams_of[13], 71), 0)
    log_decay = draw_log_decay(jax.random.fold_in(streams_of[13], 71), 0)
    start_state = noise(streams_of[10], (2, D_LRU), 2.0, 8.0, ((1, 4),), jnp.float32)
    w_out_pool = noise(streams_of[11], (D_POOL, D), (D_POOL + D_LRU) ** -0.5, 0.09375, ((0, 4), (1, 8)))
    w_out_lru = noise(streams_of[12], (D_LRU, D), (D_POOL + D_LRU) ** -0.5, 0.09375, ((0, 4), (1, 8)))
    return {"tokens": tokens, "norm_gain": norm_gain, "w_pool_in": w_pool_in, "w_lru_in": w_lru_in, "pool_mix": pool_mix, "conv_taps": conv_taps, "rec_gate": rec_gate, "in_gate": in_gate, "decay_rate": decay_rate, "log_decay": log_decay, "start_state": start_state, "w_out_pool": w_out_pool, "w_out_lru": w_out_lru}


epsilon = 1e-06

def box_bounds(length, span_len):
    element_offsets = jnp.arange(length, dtype=jnp.int32)
    lower_end = jnp.clip(element_offsets - span_len // 2, 0, length)
    upper_end = jnp.clip(element_offsets + span_len - span_len // 2, 0, length)
    return (lower_end, upper_end)

def box_sum(values, span_len, axis_dim):
    length = values.shape[axis_dim]
    pad_widths = [(0, 0)] * values.ndim
    pad_widths[axis_dim] = (span_len // 2, span_len // 2)
    padded = jnp.pad(values, pad_widths)
    total_sum = jnp.zeros_like(values)
    for offset in range(span_len):
        total_sum = total_sum + lax.slice_in_dim(padded, offset, offset + length, axis=axis_dim)
    return total_sum

def reference(tokens, norm_gain, w_pool_in, w_lru_in, pool_mix, conv_taps, rec_gate, in_gate, decay_rate, log_decay, start_state, w_out_pool, w_out_lru):
    values = tokens.astype(jnp.float32)
    root_mean_square_scale = lax.rsqrt(lax.optimization_barrier(jnp.mean(values * values, axis=1, keepdims=True)) + epsilon)
    normed = (values * root_mean_square_scale * norm_gain).astype(jnp.bfloat16)
    u_pool = jnp.dot(normed, w_pool_in, preferred_element_type=jnp.float32).astype(jnp.bfloat16)
    u_lru = jnp.dot(normed, w_lru_in, preferred_element_type=jnp.float32).astype(jnp.bfloat16)
    grid_pooled_image = u_pool.reshape(ROWS, GRID_W, D_POOL)
    outputs_pool = []
    for group_index in range(POOL_GROUPS):
        span_len = 2 ** (group_index + 1)
        channels = grid_pooled_image[:, :, group_index * GROUP_W:(group_index + 1) * GROUP_W].astype(jnp.float32)
        total_sum = box_sum(box_sum(channels, span_len, 0), span_len, 1)
        row_lower, row_upper = box_bounds(ROWS, span_len)
        col_lower, col_upper = box_bounds(GRID_W, span_len)
        counts = ((row_upper - row_lower)[:, None] * (col_upper - col_lower)[None, :]).astype(jnp.float32)
        pool_diff = (total_sum / counts[:, :, None] - channels).astype(jnp.bfloat16).reshape(TOKENS, GROUP_W)
        outputs_pool.append(jnp.dot(pool_diff, pool_mix[group_index], preferred_element_type=jnp.float32).astype(jnp.bfloat16))
    y_pool = jnp.concatenate(outputs_pool, axis=1)
    left_taps = CONV // 2
    padded = jnp.pad(u_lru.astype(jnp.float32), ((left_taps, CONV - 1 - left_taps), (0, 0)))
    tap_weights = conv_taps.astype(jnp.float32)
    conv_sum = padded[0:TOKENS] * tap_weights[0]
    for tap_index in range(1, CONV):
        conv_sum = conv_sum + padded[tap_index:tap_index + TOKENS] * tap_weights[tap_index]
    conv_in = conv_sum.astype(jnp.bfloat16)
    blocks = conv_in.astype(jnp.float32).reshape(TOKENS, BLOCKS, HEAD)
    drive_in = conv_in.astype(jnp.float32)
    histories = []
    for direction in range(2):
        recur_gate = jax.nn.sigmoid(jnp.einsum('tnc,ncd->tnd', blocks, rec_gate[direction].astype(jnp.float32)).reshape(TOKENS, D_LRU))
        input_gate = jax.nn.sigmoid(jnp.einsum('tnc,ncd->tnd', blocks, in_gate[direction].astype(jnp.float32)).reshape(TOKENS, D_LRU))
        log_keep = -8.0 * recur_gate * decay_rate[direction] + log_decay[direction][:, None]
        keep_rate = jnp.exp(log_keep)
        drive_term = jnp.sqrt(-jnp.expm1(2.0 * log_keep)) * input_gate * drive_in

        def recurrence_step(carried, pair_now):
            updated = pair_now[0] * carried + pair_now[1]
            return (updated, updated)
        _, history = lax.scan(recurrence_step, start_state[direction], (keep_rate, drive_term), reverse=direction == 1)
        histories.append(history)
    y_lru = (histories[0] + histories[1]).astype(jnp.bfloat16)
    mixed = jnp.dot(y_pool, w_out_pool, preferred_element_type=jnp.float32) + jnp.dot(y_lru, w_out_lru, preferred_element_type=jnp.float32)
    return mixed.astype(jnp.bfloat16)
```

```python
import functools

import jax
import jax.numpy as jnp
from jax import lax
from jax.experimental import pallas as pl
from jax.experimental.pallas import tpu as pltpu
from jax.sharding import PartitionSpec as P

POOL_GROUPS = 4
GRID_W = 32
REACH = 2 ** (POOL_GROUPS - 1)
EPSILON = 1e-06
EDGE = 16
CHUNKS = 8


def one_minus_exp(y):
    series = jnp.full_like(y, 1.0 / 40320.0)
    for factorial in (5040.0, 720.0, 120.0, 24.0, 6.0, 2.0, 1.0):
        series = series * y + 1.0 / factorial
    return jnp.where(y > -0.35, -y * series, 1.0 - jnp.exp(y))


def pool_stage(ext, mix_ref, tp, first_row, row_count, tokens):
    half = jnp.left_shift(jnp.int32(1), tp)
    reached = ext.shape[0]
    shape = (tokens, reached)
    out_tok = lax.broadcasted_iota(jnp.int32, shape, 0)
    in_tok = lax.broadcasted_iota(jnp.int32, shape, 1)
    row_step = in_tok // GRID_W - REACH - out_tok // GRID_W
    col_step = in_tok % GRID_W - out_tok % GRID_W
    inside = (row_step >= -half) & (row_step < half) & (col_step >= -half) & (col_step < half)
    box = jnp.where(inside, 1.0, 0.0).astype(jnp.bfloat16)
    total = jnp.dot(box, ext[...], preferred_element_type=jnp.float32)
    tok = lax.broadcasted_iota(jnp.int32, (tokens, 1), 0)
    row, col = first_row + tok // GRID_W, tok % GRID_W
    rows = jnp.minimum(row + half, row_count) - jnp.maximum(row - half, 0)
    cols = jnp.minimum(col + half, GRID_W) - jnp.maximum(col - half, 0)
    count = (rows * cols).astype(jnp.float32)
    own = ext[REACH * GRID_W : REACH * GRID_W + tokens].astype(jnp.float32)
    diff = (total / count - own).astype(jnp.bfloat16)
    return jnp.dot(diff, mix_ref[0], preferred_element_type=jnp.float32).astype(jnp.bfloat16)


def gate_stage(wide, taps_ref, rec_ref, ing_ref, rate_ref, logd_ref, keep, drive, tokens):
    tap_count = taps_ref.shape[0]
    taps = taps_ref[...].astype(jnp.float32)
    left = tap_count // 2
    blocks, head = rec_ref.shape[1:3]
    for block in range(blocks):
        lanes = slice(block * head, (block + 1) * head)
        conv = wide[EDGE - left : EDGE - left + tokens, lanes] * taps[0:1, lanes]
        for k in range(1, tap_count):
            at = EDGE - left + k
            conv = conv + wide[at : at + tokens, lanes] * taps[k : k + 1, lanes]
        conv_in = conv.astype(jnp.bfloat16)
        drive_in = conv_in.astype(jnp.float32)
        for d in range(2):
            rec = jax.nn.sigmoid(
                jnp.dot(conv_in, rec_ref[d, block], preferred_element_type=jnp.float32)
            )
            ing = jax.nn.sigmoid(
                jnp.dot(conv_in, ing_ref[d, block], preferred_element_type=jnp.float32)
            )
            log_keep = -8.0 * rec * rate_ref[d : d + 1, lanes] + logd_ref[:, d : d + 1]
            keep[d * blocks + block] = jnp.exp(log_keep)
            drive[d * blocks + block] = jnp.sqrt(one_minus_exp(2.0 * log_keep)) * ing * drive_in


def scan_stage(keep, drive, tokens):
    steps = tokens // CHUNKS
    count, head = keep.shape[0], keep.shape[2]

    def step(i, carry):
        after = []
        for k in range(count):
            at = i if k < count // 2 else steps - 1 - i
            rows = pl.ds(at, CHUNKS, stride=steps)
            a = keep[k, rows, :]
            prod = a * carry[2 * k]
            state = a * carry[2 * k + 1] + drive[k, rows, :]
            keep[k, rows, :] = prod
            drive[k, rows, :] = state
            after += [prod, state]
        return tuple(after)

    one = jnp.ones((CHUNKS, head), jnp.float32)
    zero = jnp.zeros((CHUNKS, head), jnp.float32)
    out = lax.fori_loop(0, steps, step, (one, zero) * count)
    halves = (out[:count], out[count:])
    return tuple(jnp.concatenate(half[j::2], axis=1) for half in halves for j in range(2))


def run_summary(pf, hf, pb, hb):
    fp, fh = pf[0:1], hf[0:1]
    bp, bh = pb[CHUNKS - 1 :], hb[CHUNKS - 1 :]
    for c in range(1, CHUNKS):
        fh = pf[c : c + 1] * fh + hf[c : c + 1]
        fp = fp * pf[c : c + 1]
        r = CHUNKS - 1 - c
        bh = pb[r : r + 1] * bh + hb[r : r + 1]
        bp = bp * pb[r : r + 1]
    return jnp.concatenate([fp, fh, bp, bh], axis=0)


def close_stage(keep, drive, ends, enter_f, enter_b, y_ref, tokens):
    pf, hf, pb, hb = ends
    steps = tokens // CHUNKS
    fs, bs = [enter_f], [enter_b]
    for c in range(CHUNKS - 1):
        fs.append(pf[c : c + 1] * fs[-1] + hf[c : c + 1])
        r = CHUNKS - 1 - c
        bs.append(pb[r : r + 1] * bs[-1] + hb[r : r + 1])
    blocks, head = keep.shape[0] // 2, keep.shape[2]
    for c in range(CHUNKS):
        rows = slice(c * steps, (c + 1) * steps)
        for block in range(blocks):
            lanes = slice(block * head, (block + 1) * head)
            y_ref[rows, lanes] = (
                keep[block, rows, :] * fs[c][:, lanes]
                + drive[block, rows, :]
                + keep[blocks + block, rows, :] * bs[CHUNKS - 1 - c][:, lanes]
                + drive[blocks + block, rows, :]
            ).astype(jnp.bfloat16)


def local_kernel(
    ext, lru, mix, taps, rec, ing, rate, logd, y_pool, keep, drive, summary, ends, wide, *, sp
):
    tokens = y_pool.shape[0]
    grid_rows = tokens // GRID_W
    wide[...] = lru[...].astype(jnp.float32)
    gate_stage(wide, taps, rec, ing, rate, logd, keep, drive, tokens)
    parts = scan_stage(keep, drive, tokens)
    summary[...] = run_summary(*parts)
    for k in range(4):
        ends[k] = parts[k]
    y_pool[...] = pool_stage(
        ext, mix, lax.axis_index("tp"), lax.axis_index("sp") * grid_rows, sp * grid_rows, tokens
    )


def close_kernel(keep, drive, ends, enter, y_ref):
    parts = tuple(ends[k] for k in range(4))
    close_stage(keep, drive, parts, enter[0:1], enter[1:2], y_ref, y_ref.shape[0])


def with_halo(cells, width, sp):
    ends = sp - 1
    tail, head = cells[cells.shape[0] - width :], cells[:width]
    return jnp.concatenate(
        [
            lax.ppermute(tail, "sp", [(i, i + 1) for i in range(ends)]),
            cells,
            lax.ppermute(head, "sp", [(i + 1, i) for i in range(ends)]),
        ],
        axis=0,
    )


def per_device(
    sp,
    tokens,
    norm_gain,
    w_pool_in,
    w_lru_in,
    pool_mix,
    conv_taps,
    rec_gate,
    in_gate,
    decay_rate,
    log_decay,
    start_state,
    w_out_pool,
    w_out_lru,
):
    count = tokens.shape[0]
    width = w_lru_in.shape[1]
    whole = lax.all_gather(tokens, "tp", axis=1, tiled=True)
    values = whole.astype(jnp.float32)
    scale = lax.rsqrt(jnp.mean(values * values, axis=1, keepdims=True) + EPSILON)
    normed = (values * scale * norm_gain).astype(jnp.bfloat16)
    full_lru = lax.all_gather(w_lru_in, "sp", axis=0, tiled=True)
    full_pool = lax.all_gather(w_pool_in, "sp", axis=0, tiled=True)
    u_lru = jnp.dot(normed, full_lru, preferred_element_type=jnp.float32).astype(jnp.bfloat16)
    u_pool = jnp.dot(normed, full_pool, preferred_element_type=jnp.float32).astype(jnp.bfloat16)
    ext = with_halo(u_pool, REACH * GRID_W, sp)
    lru = with_halo(u_lru, EDGE, sp)
    f32 = jnp.float32
    blocks, head = rec_gate.shape[1:3]
    vmem = pl.BlockSpec(memory_space=pltpu.VMEM)
    y_pool, keep, drive, summary, ends = pl.pallas_call(
        functools.partial(local_kernel, sp=sp),
        out_shape=(
            jax.ShapeDtypeStruct((count, width), jnp.bfloat16),
            jax.ShapeDtypeStruct((2 * blocks, count, head), f32),
            jax.ShapeDtypeStruct((2 * blocks, count, head), f32),
            jax.ShapeDtypeStruct((4, width), f32),
            jax.ShapeDtypeStruct((4, CHUNKS, width), f32),
        ),
        in_specs=[vmem] * 8,
        out_specs=(vmem,) * 5,
        scratch_shapes=[pltpu.VMEM((count + 2 * EDGE, width), f32)],
        compiler_params=pltpu.CompilerParams(vmem_limit_bytes=40 * 2**20),
    )(ext, lru, pool_mix, conv_taps, rec_gate, in_gate, decay_rate, log_decay.T)
    every = lax.all_gather(summary, "sp", axis=0, tiled=False)
    me = lax.axis_index("sp")
    enter_f, enter_b = start_state[0], start_state[1]
    for s in range(sp - 1):
        r = sp - 1 - s
        enter_f = jnp.where(s < me, every[s, 0] * enter_f + every[s, 1], enter_f)
        enter_b = jnp.where(r > me, every[r, 2] * enter_b + every[r, 3], enter_b)
    y_lru = pl.pallas_call(
        close_kernel,
        out_shape=jax.ShapeDtypeStruct((count, width), jnp.bfloat16),
        in_specs=[vmem] * 4,
        out_specs=vmem,
        compiler_params=pltpu.CompilerParams(vmem_limit_bytes=40 * 2**20),
    )(keep, drive, ends, jnp.stack([enter_f, enter_b]))
    out_pool = lax.all_gather(w_out_pool, "sp", axis=1, tiled=True)
    out_lru = lax.all_gather(w_out_lru, "sp", axis=1, tiled=True)
    partial = jnp.dot(y_pool, out_pool, preferred_element_type=f32) + jnp.dot(
        y_lru, out_lru, preferred_element_type=f32
    )
    return lax.psum_scatter(
        partial.astype(jnp.bfloat16), "tp", scatter_dimension=0, tiled=True
    )


def solution(mesh):
    placed = (
        P("sp", "tp"),
        P(),
        P("sp", "tp"),
        P("sp", "tp"),
        P("tp", None, None),
        P(None, "tp"),
        P(None, "tp", None, None),
        P(None, "tp", None, None),
        P(None, "tp"),
        P(None, "sp"),
        P(None, "tp"),
        P("tp", "sp"),
        P("tp", "sp"),
    )
    return jax.shard_map(
        functools.partial(per_device, mesh.shape["sp"]),
        mesh=mesh,
        in_specs=placed,
        out_specs=P(("sp", "tp"), None),
        check_vma=False,
    )
```

```python
import functools

import jax
import jax.numpy as jnp
from jax import lax
from jax.experimental import pallas as pl
from jax.experimental.pallas import tpu as pltpu
from jax.sharding import PartitionSpec as P

POOL_GROUPS = 4
GRID_W = 32
REACH = 2 ** (POOL_GROUPS - 1)
EPSILON = 1e-06
EDGE = 16
CHUNKS = 8


def one_minus_exp(y):
    series = jnp.full_like(y, 1.0 / 40320.0)
    for factorial in (5040.0, 720.0, 120.0, 24.0, 6.0, 2.0, 1.0):
        series = series * y + 1.0 / factorial
    return jnp.where(y > -0.35, -y * series, 1.0 - jnp.exp(y))


def pool_stage(ext, mix_ref, tp, first_row, row_count, tokens):
    half = jnp.left_shift(jnp.int32(1), tp)
    reached = ext.shape[0]
    shape = (tokens, reached)
    out_tok = lax.broadcasted_iota(jnp.int32, shape, 0)
    in_tok = lax.broadcasted_iota(jnp.int32, shape, 1)
    row_step = in_tok // GRID_W - REACH - out_tok // GRID_W
    col_step = in_tok % GRID_W - out_tok % GRID_W
    inside = (row_step >= -half) & (row_step < half) & (col_step >= -half) & (col_step < half)
    box = jnp.where(inside, 1.0, 0.0).astype(jnp.bfloat16)
    total = jnp.dot(box, ext[...], preferred_element_type=jnp.float32)
    tok = lax.broadcasted_iota(jnp.int32, (tokens, 1), 0)
    row, col = first_row + tok // GRID_W, tok % GRID_W
    rows = jnp.minimum(row + half, row_count) - jnp.maximum(row - half, 0)
    cols = jnp.minimum(col + half, GRID_W) - jnp.maximum(col - half, 0)
    count = (rows * cols).astype(jnp.float32)
    own = ext[REACH * GRID_W : REACH * GRID_W + tokens].astype(jnp.float32)
    diff = (total / count - own).astype(jnp.bfloat16)
    return jnp.dot(diff, mix_ref[0], preferred_element_type=jnp.float32).astype(jnp.bfloat16)


def gate_stage(wide, taps_ref, rec_ref, ing_ref, rate_ref, logd_ref, keep, drive, tokens):
    tap_count = taps_ref.shape[0]
    taps = taps_ref[...].astype(jnp.float32)
    left = tap_count // 2
    blocks, head = rec_ref.shape[1:3]
    for block in range(blocks):
        lanes = slice(block * head, (block + 1) * head)
        conv = wide[EDGE - left : EDGE - left + tokens, lanes] * taps[0:1, lanes]
        for k in range(1, tap_count):
            at = EDGE - left + k
            conv = conv + wide[at : at + tokens, lanes] * taps[k : k + 1, lanes]
        conv_in = conv.astype(jnp.bfloat16)
        drive_in = conv_in.astype(jnp.float32)
        for d in range(2):
            rec = jax.nn.sigmoid(
                jnp.dot(conv_in, rec_ref[d, block], preferred_element_type=jnp.float32)
            )
            ing = jax.nn.sigmoid(
                jnp.dot(conv_in, ing_ref[d, block], preferred_element_type=jnp.float32)
            )
            log_keep = -8.0 * rec * rate_ref[d : d + 1, lanes] + logd_ref[:, d : d + 1]
            keep[d * blocks + block] = jnp.exp(log_keep)
            drive[d * blocks + block] = jnp.sqrt(one_minus_exp(2.0 * log_keep)) * ing * drive_in


def scan_stage(keep, drive, tokens):
    steps = tokens // CHUNKS
    count, head = keep.shape[0], keep.shape[2]

    def step(i, carry):
        after = []
        for k in range(count):
            at = i if k < count // 2 else steps - 1 - i
            rows = pl.ds(at, CHUNKS, stride=steps)
            a = keep[k, rows, :]
            prod = a * carry[2 * k]
            state = a * carry[2 * k + 1] + drive[k, rows, :]
            keep[k, rows, :] = prod
            drive[k, rows, :] = state
            after += [prod, state]
        return tuple(after)

    one = jnp.ones((CHUNKS, head), jnp.float32)
    zero = jnp.zeros((CHUNKS, head), jnp.float32)
    out = lax.fori_loop(0, steps, step, (one, zero) * count)
    halves = (out[:count], out[count:])
    return tuple(jnp.concatenate(half[j::2], axis=1) for half in halves for j in range(2))


def run_summary(pf, hf, pb, hb):
    fp, fh = pf[0:1], hf[0:1]
    bp, bh = pb[CHUNKS - 1 :], hb[CHUNKS - 1 :]
    for c in range(1, CHUNKS):
        fh = pf[c : c + 1] * fh + hf[c : c + 1]
        fp = fp * pf[c : c + 1]
        r = CHUNKS - 1 - c
        bh = pb[r : r + 1] * bh + hb[r : r + 1]
        bp = bp * pb[r : r + 1]
    return jnp.concatenate([fp, fh, bp, bh], axis=0)


def close_stage(keep, drive, ends, enter_f, enter_b, y_ref, tokens):
    pf, hf, pb, hb = ends
    steps = tokens // CHUNKS
    fs, bs = [enter_f], [enter_b]
    for c in range(CHUNKS - 1):
        fs.append(pf[c : c + 1] * fs[-1] + hf[c : c + 1])
        r = CHUNKS - 1 - c
        bs.append(pb[r : r + 1] * bs[-1] + hb[r : r + 1])
    blocks, head = keep.shape[0] // 2, keep.shape[2]
    for c in range(CHUNKS):
        rows = slice(c * steps, (c + 1) * steps)
        for block in range(blocks):
            lanes = slice(block * head, (block + 1) * head)
            y_ref[rows, lanes] = (
                keep[block, rows, :] * fs[c][:, lanes]
                + drive[block, rows, :]
                + keep[blocks + block, rows, :] * bs[CHUNKS - 1 - c][:, lanes]
                + drive[blocks + block, rows, :]
            ).astype(jnp.bfloat16)


def remote(src, dst, send_sem, recv_sem, axis, index):
    return pltpu.make_async_remote_copy(
        src_ref=src,
        dst_ref=dst,
        send_sem=send_sem,
        recv_sem=recv_sem,
        device_id={axis: index},
        device_id_type=pl.DeviceIdType.MESH,
    )


class BlockGather:
    def __init__(self, buf, sems, me, sp):
        self.buf, self.sems = buf, sems
        self.line = sp // 2
        self.a, self.b = me // 2, me % 2

    def copy(self, origin, other, send, recv, target):
        block = self.buf.at[origin * 2 + other]
        return remote(
            block, block, self.sems.at[send, origin], self.sems.at[recv, origin], "sp", target
        )

    def right(self, o):
        return self.copy(o, self.b, 0, 3, (self.a + 1) * 2 + self.b)

    def left(self, o):
        return self.copy(o, self.b, 1, 3, (self.a - 1) * 2 + self.b)

    def across(self, o):
        return self.copy(o, self.b, 2, 4, self.a * 2 + 1 - self.b)

    def landed(self, o):
        return self.copy(o, 1 - self.b, 2, 4, self.a * 2 + 1 - self.b)

    def start(self):
        a = self.a

        @pl.when(a < self.line - 1)
        def _():
            self.right(a).start()

        @pl.when(a > 0)
        def _():
            self.left(a).start()

        self.across(a).start()

    def step(self, d):
        a, line = self.a, self.line
        low, high = a - d, a + d

        @pl.when(low >= 0)
        def _():
            self.right(low).wait_recv()

            @pl.when(a < line - 1)
            def _():
                self.right(low).start()

            self.across(low).start()

        @pl.when(high < line)
        def _():
            self.left(high).wait_recv()

            @pl.when(a > 0)
            def _():
                self.left(high).start()

            self.across(high).start()

    def both(self, d, use, wait=False, other=None):
        a = self.a
        side = self.b if other is None else other
        for origin, there in ((a - d, a - d >= 0), (a + d, (a + d < self.line) & (d > 0))):

            @pl.when(there)
            def _(origin=origin):
                if wait:
                    self.landed(origin).wait_recv()
                use(origin * 2 + side)

    def finish(self):
        a, line = self.a, self.line

        @pl.loop(0, line)
        def _(o):
            @pl.when((o <= a) & (a < line - 1))
            def _():
                self.right(o).wait_send()

            @pl.when((o >= a) & (a > 0))
            def _():
                self.left(o).wait_send()

            self.across(o).wait_send()


def layer_kernel(
    tok,
    gain,
    wpi,
    wli,
    mix,
    taps,
    rec,
    ing,
    rate,
    logd,
    start,
    wpo,
    wlo,
    out,
    toks,
    normed,
    win,
    wout,
    acc,
    ext,
    edge,
    ulru,
    wide,
    keep,
    drive,
    mine,
    sums,
    y_pool,
    y_lru,
    part,
    red,
    own_sem,
    tok_sem,
    in_sem,
    out_sem,
    halo_sem,
    sum_sem,
    red_sem,
    *,
    sp,
    tp,
):
    f32 = jnp.float32
    me, t = lax.axis_index("sp"), lax.axis_index("tp")
    count, local = tok.shape
    depth, wide_out = wpi.shape[0], wpo.shape[1]
    share = count // tp
    halo = REACH * GRID_W

    owns = [
        pltpu.make_async_copy(src, dst, own_sem.at[k])
        for k, (src, dst) in enumerate(
            (
                (wpi, win.at[me, 0]),
                (wli, win.at[me, 1]),
                (tok, toks.at[t]),
                (wpo, wout.at[me, 0]),
                (wlo, wout.at[me, 1]),
            )
        )
    ]
    for own in owns:
        own.start()

    def tok_copy(k, source, target):
        return remote(tok, toks.at[source], tok_sem.at[0, k], tok_sem.at[1, k], "tp", target)

    for k in range(1, tp):
        tok_copy(k, t, lax.rem(t + k, tp)).start()
    owns[0].wait()
    owns[1].wait()
    first = BlockGather(win, in_sem, me, sp)
    line = first.line
    first.start()
    early = min(3, line)
    for d in range(1, early):
        first.step(d)

    owns[2].wait()
    for k in range(1, tp):
        source = lax.rem(t - k + tp, tp)
        tok_copy(k, source, source).wait_recv()
    square = jnp.zeros((count, 1), f32)
    for p in range(tp):
        v = toks[p].astype(f32)
        square = square + jnp.sum(v * v, axis=1, keepdims=True)
    scale = lax.rsqrt(square / (tp * local) + EPSILON)
    for p in range(tp):
        for q in range(local // depth):
            v = toks[p, :, q * depth : (q + 1) * depth].astype(f32)
            at = p * local + q * depth
            normed[p * (local // depth) + q] = (
                v * scale * gain[:, at : at + depth]
            ).astype(jnp.bfloat16)

    acc[...] = jnp.zeros_like(acc)

    def use_in(block):
        for j in range(2):
            acc[j] += jnp.dot(normed[block], win[block, j], preferred_element_type=f32)

    @pl.loop(0, early)
    def _(d):
        first.both(d, use_in)

    @pl.loop(early, line)
    def _(d):
        first.step(d)
        first.both(d, use_in)

    @pl.loop(0, line)
    def _(d):
        first.both(d, use_in, wait=True, other=1 - first.b)

    ext[halo : halo + count] = acc[0].astype(jnp.bfloat16)
    ulru[...] = acc[1].astype(jnp.bfloat16)

    def to_next(part_of):
        if part_of == 0:
            src, dst = ext.at[pl.ds(count, halo)], ext.at[pl.ds(0, halo)]
        else:
            src, dst = ulru.at[pl.ds(count - EDGE, EDGE)], edge.at[0]
        return remote(src, dst, halo_sem.at[0, part_of], halo_sem.at[1, part_of], "sp", me + 1)

    def to_prev(part_of):
        k = 2 + part_of
        if part_of == 0:
            src, dst = ext.at[pl.ds(halo, halo)], ext.at[pl.ds(halo + count, halo)]
        else:
            src, dst = ulru.at[pl.ds(0, EDGE)], edge.at[1]
        return remote(src, dst, halo_sem.at[0, k], halo_sem.at[1, k], "sp", me - 1)

    for part_of in (1, 0):

        @pl.when(me < sp - 1)
        def _(part_of=part_of):
            to_next(part_of).start()

        @pl.when(me > 0)
        def _(part_of=part_of):
            to_prev(part_of).start()

    owns[3].wait()
    owns[4].wait()
    second = BlockGather(wout, out_sem, me, sp)
    second.start()

    @pl.when(me == 0)
    def _():
        edge[0] = jnp.zeros(edge.shape[1:], edge.dtype)
        ext[0:halo] = jnp.zeros((halo, ext.shape[1]), ext.dtype)

    @pl.when(me == sp - 1)
    def _():
        edge[1] = jnp.zeros(edge.shape[1:], edge.dtype)
        ext[halo + count :] = jnp.zeros((halo, ext.shape[1]), ext.dtype)

    def halo_wait(part_of):
        @pl.when(me > 0)
        def _():
            to_next(part_of).wait_recv()

        @pl.when(me < sp - 1)
        def _():
            to_prev(part_of).wait_recv()

    halo_wait(1)
    wide[0:EDGE] = edge[0].astype(f32)
    wide[EDGE : EDGE + count] = ulru[...].astype(f32)
    wide[EDGE + count :] = edge[1].astype(f32)
    gate_stage(wide, taps, rec, ing, rate, logd, keep, drive, count)
    ends = scan_stage(keep, drive, count)
    mine[0:4] = run_summary(*ends)
    mine[4:8] = jnp.zeros((4, mine.shape[1]), f32)
    sums[me] = mine[...]

    def sum_copy(k, source, target):
        return remote(mine, sums.at[source], sum_sem.at[0, k], sum_sem.at[1, k], "sp", target)

    for k in range(1, sp):
        sum_copy(k, me, lax.rem(me + k, sp)).start()
    halo_wait(0)
    grid_rows = count // GRID_W
    y_pool[...] = pool_stage(ext, mix, t, me * grid_rows, sp * grid_rows, count)
    if line > 1:
        second.step(1)
    for k in range(1, sp):
        source = lax.rem(me - k + sp, sp)
        sum_copy(k, source, source).wait_recv()
    enter_f, enter_b = start[0:1], start[1:2]
    for s in range(sp - 1):
        r = sp - 1 - s
        enter_f = jnp.where(s < me, sums[s, 0:1] * enter_f + sums[s, 1:2], enter_f)
        enter_b = jnp.where(r > me, sums[r, 2:3] * enter_b + sums[r, 3:4], enter_b)
    close_stage(keep, drive, ends, enter_f, enter_b, y_lru, count)

    def red_copy(k, block, target):
        rows = pl.ds(pl.multiple_of(target * share, share), share)
        return remote(
            part.at[block, rows],
            red.at[k, block],
            red_sem.at[0, k, block],
            red_sem.at[1, k, block],
            "tp",
            target,
        )

    def use_out(block):
        part[block] = (
            jnp.dot(y_pool[...], wout[block, 0], preferred_element_type=f32)
            + jnp.dot(y_lru[...], wout[block, 1], preferred_element_type=f32)
        ).astype(jnp.bfloat16)
        for k in range(1, tp):
            red_copy(k, block, lax.rem(t + k, tp)).start()

    ready = min(2, line)

    @pl.loop(0, ready)
    def _(d):
        second.both(d, use_out)

    @pl.loop(ready, line)
    def _(d):
        second.step(d)
        second.both(d, use_out)

    @pl.loop(0, line)
    def _(d):
        second.both(d, use_out, wait=True, other=1 - second.b)

    rows = pl.ds(pl.multiple_of(t * share, share), share)
    for block in range(sp):
        total = part[block, rows, :].astype(f32)
        for k in range(1, tp):
            red_copy(k, block, lax.rem(t + k, tp)).wait_recv()
            total = total + red[k, block].astype(f32)
        out[:, block * wide_out : (block + 1) * wide_out] = total.astype(out.dtype)

    first.finish()
    second.finish()
    for k in range(1, tp):
        tok_copy(k, t, lax.rem(t + k, tp)).wait_send()
    for k in range(1, sp):
        sum_copy(k, me, lax.rem(me + k, sp)).wait_send()
    for part_of in range(2):

        @pl.when(me < sp - 1)
        def _(part_of=part_of):
            to_next(part_of).wait_send()

        @pl.when(me > 0)
        def _(part_of=part_of):
            to_prev(part_of).wait_send()

    @pl.loop(0, sp)
    def _(block):
        for k in range(1, tp):
            red_copy(k, block, lax.rem(t + k, tp)).wait_send()


def per_device(
    sp,
    tp,
    tokens,
    norm_gain,
    w_pool_in,
    w_lru_in,
    pool_mix,
    conv_taps,
    rec_gate,
    in_gate,
    decay_rate,
    log_decay,
    start_state,
    w_out_pool,
    w_out_lru,
):
    count, local = tokens.shape
    depth, width = w_lru_in.shape
    wide_out = w_out_pool.shape[1]
    blocks, head = rec_gate.shape[1:3]
    f32, bf16 = jnp.float32, jnp.bfloat16
    vmem = pl.BlockSpec(memory_space=pltpu.VMEM)
    far = pl.BlockSpec(memory_space=pl.ANY)
    share = count // tp
    dma = pltpu.SemaphoreType.DMA
    return pl.pallas_call(
        functools.partial(layer_kernel, sp=sp, tp=tp),
        out_shape=jax.ShapeDtypeStruct((share, wide_out * sp), bf16),
        in_specs=[far, vmem, far, far] + [vmem] * 7 + [far, far],
        out_specs=vmem,
        scratch_shapes=[
            pltpu.VMEM((tp, count, local), bf16),
            pltpu.VMEM((sp, count, depth), bf16),
            pltpu.VMEM((sp, 2, depth, width), bf16),
            pltpu.VMEM((sp, 2, width, wide_out), bf16),
            pltpu.VMEM((2, count, width), f32),
            pltpu.VMEM((count + 2 * REACH * GRID_W, width), bf16),
            pltpu.VMEM((2, EDGE, width), bf16),
            pltpu.VMEM((count, width), bf16),
            pltpu.VMEM((count + 2 * EDGE, width), f32),
            pltpu.VMEM((2 * blocks, count, head), f32),
            pltpu.VMEM((2 * blocks, count, head), f32),
            pltpu.VMEM((8, width), f32),
            pltpu.VMEM((sp, 8, width), f32),
            pltpu.VMEM((count, width), bf16),
            pltpu.VMEM((count, width), bf16),
            pltpu.VMEM((sp, count, wide_out), bf16),
            pltpu.VMEM((tp, sp, share, wide_out), bf16),
            dma((5,)),
            dma((2, tp)),
            dma((5, sp // 2)),
            dma((5, sp // 2)),
            dma((2, 4)),
            dma((2, sp)),
            dma((2, tp, sp)),
        ],
        compiler_params=pltpu.CompilerParams(
            has_side_effects=True, vmem_limit_bytes=60 * 2**20
        ),
    )(
        tokens,
        norm_gain[None],
        w_pool_in,
        w_lru_in,
        pool_mix,
        conv_taps,
        rec_gate,
        in_gate,
        decay_rate,
        log_decay.T,
        start_state,
        w_out_pool,
        w_out_lru,
    )


def solution(mesh):
    placed = (
        P("sp", "tp"),
        P(),
        P("sp", "tp"),
        P("sp", "tp"),
        P("tp", None, None),
        P(None, "tp"),
        P(None, "tp", None, None),
        P(None, "tp", None, None),
        P(None, "tp"),
        P(None, "sp"),
        P(None, "tp"),
        P("tp", "sp"),
        P("tp", "sp"),
    )
    return jax.shard_map(
        functools.partial(per_device, mesh.shape["sp"], mesh.shape["tp"]),
        mesh=mesh,
        in_specs=placed,
        out_specs=P(("sp", "tp"), None),
        check_vma=False,
    )
```
